32 devices in a mesh: fs: 8 (over z, y), tp: 4 (over x, core).
Axes of the slice: x: 2, y: 2, z: 4, core: 2. Of those that a mesh axis runs over, the one named last changes fastest.
Arguments:
- tokens: bfloat16 [6144, 2048], P('fs', 'tp'), may hold values from -40 to 40
- gain_one: float32 [2048], P('tp'), may hold values from 0.1 to 1.9
- w_gate: float32 [2048, 3072], P('fs', 'tp'), may hold values from -0.125 to 0.125
- w_up: float32 [2048, 3072], P('fs', 'tp'), may hold values from -0.125 to 0.125
- w_down: float32 [3072, 2048], P('tp', 'fs'), may hold values from -0.109375 to 0.109375
- scale_gate: float32 [3072], P('tp'), may hold values from 0.5 to 2
- scale_up: float32 [3072], P('tp'), may hold values from 0.5 to 2
- scale_down: float32 [2048], P('tp'), may hold values from 0.5 to 2
- gain_mix: float32 [2048], P('tp'), may hold values from 0.1 to 1.9
- w_query: float32 [2048, 2048], P('fs', 'tp'), may hold values from -0.125 to 0.125
- w_key: float32 [2048, 2048], P('fs', 'tp'), may hold values from -0.125 to 0.125
- w_value: float32 [2048, 2048], P('fs', 'tp'), may hold values from -0.125 to 0.125
- w_outgate: float32 [2048, 2048], P('fs', 'tp'), may hold values from -0.125 to 0.125
- scale_query: float32 [2048], P('tp'), may hold values from 0.5 to 2
- scale_key: float32 [2048], P('tp'), may hold values from 0.5 to 2
- scale_value: float32 [2048], P('tp'), may hold values from 0.5 to 2
- scale_outgate: float32 [2048], P('tp'), may hold values from 0.5 to 2
- ret_gain: float32 [2048], P('tp'), may hold values from 0.1 to 1.9
- decay_rate: float32 [8], P('tp'), may hold values from 0 to 2
- w_mix: float32 [2048, 2048], P('tp', 'fs'), may hold values from -0.125 to 0.125
- scale_mix: float32 [2048], P('tp'), may hold values from 0.5 to 2
- gain_two: float32 [2048], P('tp'), may hold values from 0.1 to 1.9
Outputs:
- layer_out: bfloat16 [6144, 2048], P('fs', 'tp')
The draws below stay inside these ranges and needn't reach their ends.
All inputs are finite; a program needn't handle non-finite values.
Results may differ from the reference program's by a relative error of at most 0.022.
Values may be sent and summed in bfloat16 or wider, within the bound.
A program may use at most 128 MiB of HBM per device.

```python
import math
import jax
import jax.numpy as jnp
from jax import lax

D = 2048
FF = 3072
HEADS = 8
LEN = 256
BLK = 128
RW = 2048
TOKENS = 6144
N_TP = 4


def draw_tokens(key, part):
    base = jax.random.normal(jax.random.fold_in(key, 13), (TOKENS, D), jnp.float32)
    logs = jax.random.uniform(jax.random.fold_in(key, 14), (TOKENS, 8), jnp.float32, -1.2, 1.2)
    factors = jnp.repeat(jnp.exp(logs), D // 8, axis=1)
    return (base * factors).astype(jnp.bfloat16)


def draw_decay_rate(key, part):
    picks = jax.random.randint(jax.random.fold_in(key, 21), (HEADS,), 0, 2)
    quick = jax.random.uniform(jax.random.fold_in(key, 22), (HEADS,), jnp.float32, 4.0 / BLK, 16.0 / BLK)
    slower = jax.random.uniform(jax.random.fold_in(key, 23), (HEADS,), jnp.float32, 0.3 / LEN, 2.3 / LEN)
    return jnp.where(picks == 1, quick, slower)


def steps_of(rng, extent, split, low, high):
    factor_of, own = 1.0, jax.random.fold_in(rng, 6)
    for position, blocks in split:
        heights = jnp.exp(jax.random.uniform(jax.random.fold_in(own, position), (blocks,), jnp.float32, low / len(split), high / len(split)))
        factor_of = factor_of * jnp.repeat(heights, extent[position] // blocks).reshape([-1 if axis == position else 1 for axis in range(len(extent))])
    return factor_of


def centred(rng, dims, deviation, most, split=(), held_as=jnp.bfloat16):
    array = deviation * jax.random.normal(rng, dims, jnp.float32)
    if split:
        array = array * steps_of(rng, dims, split, -0.22, 0.18)
    return jnp.clip(array, -most, most).astype(held_as)


def setup_inputs(seed: int = 0) -> dict:
    seeds = jax.random.split(jax.random.key(seed), 23)
    tokens = draw_tokens(jax.random.fold_in(seeds[22], 71), 0)
    gain_one = jnp.clip(1.0 + 0.18 * jax.random.normal(seeds[1], (D,), jnp.float32), 0.1, 1.9)
    w_gate = centred(seeds[2], (D, FF), D ** -0.5, 0.125, ((0, 8), (1, 4)), jnp.float32)
    w_up = centred(seeds[3], (D, FF), D ** -0.5, 0.125, ((0, 8), (1, 4)), jnp.float32)
    w_down = centred(seeds[4], (FF, D), FF ** -0.5, 0.109375, ((0, 4), (1, 8)), jnp.float32)
    scale_gate = jnp.clip(jnp.exp(math.log(2.0) - 1.3862944 * jax.random.uniform(seeds[5], (FF,), jnp.float32) ** steps_of(seeds[5], (FF,), ((0, 4),), -0.2, 0.2)), 0.5, 2.0)
    scale_up = jnp.clip(jnp.exp(math.log(2.0) - 1.3862944 * jax.random.uniform(seeds[6], (FF,), jnp.float32) ** steps_of(seeds[6], (FF,), ((0, 4),), -0.2, 0.2)), 0.5, 2.0)
    scale_down = jnp.clip(jnp.exp(math.log(2.0) - 1.3862944 * jax.random.uniform(seeds[7], (D,), jnp.float32) ** steps_of(seeds[7], (D,), ((0, 4),), -0.2, 0.2)), 0.5, 2.0)
    gain_mix = jnp.clip(1.0 + 0.18 * jax.random.normal(seeds[8], (D,), jnp.float32), 0.1, 1.9)
    w_query = centred(seeds[9], (D, RW), D ** -0.5, 0.125, ((0, 8), (1, 4)), jnp.float32)
    w_key = centred(seeds[10], (D, RW), D ** -0.5, 0.125, ((0, 8), (1, 4)), jnp.float32)
    w_value = centred(seeds[11], (D, RW), D ** -0.5, 0.125, ((0, 8), (1, 4)), jnp.float32)
    w_outgate = centred(seeds[12], (D, RW), D ** -0.5, 0.125, ((0, 8), (1, 4)), jnp.float32)
    scale_query = jnp.clip(jnp.exp(math.log(2.0) - 1.3862944 * jax.random.uniform(seeds[13], (RW,), jnp.float32) ** steps_of(seeds[13], (RW,), ((0, 4),), -0.2, 0.2)), 0.5, 2.0)
    scale_key = jnp.clip(jnp.exp(math.log(2.0) - 1.3862944 * jax.random.uniform(seeds[14], (RW,), jnp.float32) ** steps_of(seeds[14], (RW,), ((0, 4),), -0.2, 0.2)), 0.5, 2.0)
    scale_value = jnp.clip(jnp.exp(math.log(2.0) - 1.3862944 * jax.random.uniform(seeds[15], (RW,), jnp.float32) ** steps_of(seeds[15], (RW,), ((0, 4),), -0.2, 0.2)), 0.5, 2.0)
    scale_outgate = jnp.clip(jnp.exp(math.log(2.0) - 1.3862944 * jax.random.uniform(seeds[16], (RW,), jnp.float32) ** steps_of(seeds[16], (RW,), ((0, 4),), -0.2, 0.2)), 0.5, 2.0)
    ret_gain = jnp.clip(1.0 + 0.18 * jax.random.normal(seeds[17], (RW,), jnp.float32), 0.1, 1.9)
    decay_rate = draw_decay_rate(jax.random.fold_in(seeds[22], 71), 0)
    w_mix = centred(seeds[19], (RW, D), RW ** -0.5, 0.125, ((0, 4), (1, 8)), jnp.float32)
    scale_mix = jnp.clip(jnp.exp(math.log(2.0) - 1.3862944 * jax.random.uniform(seeds[20], (D,), jnp.float32) ** steps_of(seeds[20], (D,), ((0, 4),), -0.2, 0.2)), 0.5, 2.0)
    gain_two = jnp.clip(1.0 + 0.18 * jax.random.normal(seeds[21], (D,), jnp.float32), 0.1, 1.9)
    return dict(tokens=tokens, gain_one=gain_one, w_gate=w_gate, w_up=w_up, w_down=w_down, scale_gate=scale_gate, scale_up=scale_up, scale_down=scale_down, gain_mix=gain_mix, w_query=w_query, w_key=w_key, w_value=w_value, w_outgate=w_outgate, scale_query=scale_query, scale_key=scale_key, scale_value=scale_value, scale_outgate=scale_outgate, ret_gain=ret_gain, decay_rate=decay_rate, w_mix=w_mix, scale_mix=scale_mix, gain_two=gain_two)


EPS = 1e-06
HEAD_EPS = 0.1

def rms_rows(hidden_in, norm_gain):
    widened = hidden_in.astype(jnp.float32)
    scaled = widened * lax.rsqrt(lax.optimization_barrier(jnp.mean(widened * widened, axis=1, keepdims=True)) + EPS) * norm_gain
    return scaled.astype(jnp.bfloat16)

def project(features, weight, column_scale):
    return jnp.dot(features, weight.astype(jnp.bfloat16), preferred_element_type=jnp.float32) * column_scale

def split_sum(left, weight, parts):
    width = left.shape[1] // parts

    def add_block(index, total):
        start = (index * width).astype(jnp.int32)
        columns = lax.dynamic_slice_in_dim(left, start, width, 1)
        block = lax.dynamic_slice_in_dim(weight, start, width, 0).astype(jnp.bfloat16)
        partial_value = jnp.dot(columns, block, preferred_element_type=jnp.float32).astype(jnp.bfloat16)
        partial_value = lax.optimization_barrier(partial_value)
        return total + partial_value.astype(jnp.float32)
    return lax.fori_loop(0, parts, add_block, jnp.zeros((left.shape[0], weight.shape[1]), jnp.float32))

def feed_forward(features, w_gate, w_up, w_down, scale_gate, scale_up, scale_down):
    gate_pre = project(features, w_gate, scale_gate)
    up_pre = project(features, w_up, scale_up)
    hidden = (jax.nn.silu(gate_pre) * up_pre).astype(jnp.bfloat16)
    return split_sum(hidden, w_down, N_TP) * scale_down

def rotate_pairs(values):
    paired = values.reshape(values.shape[:-1] + (values.shape[-1] // 2, 2))
    return jnp.stack((-paired[..., 1], paired[..., 0]), axis=-1).reshape(values.shape)

def retain(query_rows, key_rows, value_rows, decay_rate, length, block):
    highest = lax.Precision.HIGHEST
    total_rows = query_rows.shape[0]
    heads = decay_rate.shape[0]
    head_size = query_rows.shape[1] // heads
    sequences = total_rows // length
    nblocks = length // block

    def split_heads(values):
        return values.astype(jnp.float32).reshape(sequences, length, heads, head_size)
    freq = 1.0 / 10000.0 ** jnp.linspace(0.0, 1.0, head_size // 2, dtype=jnp.float32)
    freq = jnp.repeat(freq, 2)
    angles = jnp.arange(length, dtype=jnp.float32)[:, None] * freq[None, :]
    sines = jnp.sin(angles)[None, :, None, :]
    cosines = jnp.cos(angles)[None, :, None, :]
    queries = split_heads(query_rows)
    queries = queries * cosines + rotate_pairs(queries) * sines
    keys_all = split_heads(key_rows) * head_size ** (-0.5)
    keys_all = keys_all * cosines + rotate_pairs(keys_all) * sines
    values_all = split_heads(value_rows)
    log_decay = -decay_rate.astype(jnp.float32)
    offsets = jnp.arange(block, dtype=jnp.float32)
    distance = offsets[:, None] - offsets[None, :]
    inside = jnp.where(distance >= 0, jnp.exp(log_decay[:, None, None] * jnp.maximum(distance, 0.0)), 0.0)
    query_decay = jnp.exp(log_decay[None, :] * (offsets[:, None] + 1.0))
    key_decay = jnp.exp(log_decay[None, :] * (block - 1.0 - offsets[:, None]))
    block_decay = jnp.exp(log_decay * block)

    def to_blocks(values):
        return jnp.moveaxis(values.reshape(sequences, nblocks, block, heads, head_size), 1, 0)

    def advance(carried, pieces):
        query_blk, key_blk, value_blk = pieces
        scores = jnp.einsum('snhd,smhd->shnm', query_blk, key_blk, precision=highest) * inside
        within = jnp.einsum('shnm,smhe->snhe', scores, value_blk, precision=highest)
        across = jnp.einsum('snhd,shde->snhe', query_blk, carried, precision=highest) * query_decay[None, :, :, None]
        weighted = key_blk * key_decay[None, :, :, None]
        carried = carried * block_decay[None, :, None, None] + jnp.einsum('smhd,smhe->shde', weighted, value_blk, precision=highest)
        return (carried, within + across)
    initial = jnp.zeros((sequences, heads, head_size, head_size), jnp.float32)
    _, results = lax.scan(advance, initial, (to_blocks(queries), to_blocks(keys_all), to_blocks(values_all)))
    results = jnp.moveaxis(results, 0, 1).reshape(sequences, length, heads, head_size)
    results = results * lax.rsqrt(lax.optimization_barrier(jnp.mean(results * results, axis=-1, keepdims=True)) + HEAD_EPS)
    return results.reshape(total_rows, heads * head_size)

def reference(tokens, gain_one, w_gate, w_up, w_down, scale_gate, scale_up, scale_down, gain_mix, w_query, w_key, w_value, w_outgate, scale_query, scale_key, scale_value, scale_outgate, ret_gain, decay_rate, w_mix, scale_mix, gain_two):
    ffn_one = feed_forward(rms_rows(tokens, gain_one), w_gate, w_up, w_down, scale_gate, scale_up, scale_down)
    first = (tokens.astype(jnp.float32) + 0.5 * ffn_one).astype(jnp.bfloat16)
    features = rms_rows(first, gain_mix)
    query_rows = project(features, w_query, scale_query).astype(jnp.bfloat16)
    key_rows = project(features, w_key, scale_key).astype(jnp.bfloat16)
    value_rows = project(features, w_value, scale_value).astype(jnp.bfloat16)
    outgate_rows = project(features, w_outgate, scale_outgate).astype(jnp.bfloat16)
    retained = retain(query_rows, key_rows, value_rows, decay_rate, LEN, BLK)
    mixed = (retained * ret_gain * jax.nn.silu(outgate_rows.astype(jnp.float32))).astype(jnp.bfloat16)
    second = (first.astype(jnp.float32) + split_sum(mixed, w_mix, N_TP) * scale_mix).astype(jnp.bfloat16)
    ffn_two = feed_forward(rms_rows(second, gain_two), w_gate, w_up, w_down, scale_gate, scale_up, scale_down)
    return (second.astype(jnp.float32) + 0.5 * ffn_two).astype(jnp.bfloat16)
```

```python
import functools

import jax
import jax.numpy as jnp
import numpy as np
from jax import lax
from jax.experimental import pallas as pl
from jax.experimental.pallas import tpu as pltpu
from jax.sharding import PartitionSpec as P

LEN = 256
EPS = 1e-06
HEAD_EPS = 0.1
MESH = pl.DeviceIdType.MESH
BF16 = jnp.bfloat16
F32 = jnp.float32


def rows_of(ref, piece, rows):
    return ref.at[pl.ds(piece * rows, rows)]


def cols_at(index, width):
    return pl.ds(pl.multiple_of(index * width, width), width)


def remote(src, dst, send_sem, recv_sem, axis, target):
    return pltpu.make_async_remote_copy(
        src_ref=src,
        dst_ref=dst,
        send_sem=send_sem,
        recv_sem=recv_sem,
        device_id={axis: target},
        device_id_type=MESH,
    )


class TpGather:
    def __init__(self, ntp, src, out, sends, forwards, recvs, pieces):
        self.t = lax.axis_index("tp")
        self.nx = ntp // 2
        self.core = lax.rem(self.t, 2)
        self.chip = lax.div(self.t, 2)
        self.partner = self.chip * 2 + (1 - self.core)
        self.src, self.out = src, out
        self.sends, self.forwards, self.recvs = sends, forwards, recvs
        self.pieces = pieces
        self.rows = src.shape[0] // pieces
        self.width = src.shape[1]

    def along_x(self, offset, core):
        return lax.rem(self.chip + offset, self.nx) * 2 + core

    def place(self, index, piece):
        return self.out.at[pl.ds(piece * self.rows, self.rows), cols_at(index, self.width)]

    def own_sends(self, piece):
        src = rows_of(self.src, piece, self.rows)
        copies = []
        for offset in range(self.nx - 1, -1, -1):
            target = self.along_x(offset, self.core) if offset else self.partner
            copies.append(
                remote(
                    src,
                    self.place(self.t, piece),
                    self.sends.at[offset, piece],
                    self.recvs.at[self.t, piece],
                    "tp",
                    target,
                )
            )
        return copies

    def forward(self, offset, piece):
        index = self.along_x(self.nx - offset, self.core)
        block = self.place(index, piece)
        return remote(
            block,
            block,
            self.forwards.at[offset, piece],
            self.recvs.at[index, piece],
            "tp",
            self.partner,
        )

    def arrived(self, index, piece):
        block = self.place(index, piece)
        remote(
            block,
            block,
            self.sends.at[0, piece],
            self.recvs.at[index, piece],
            "tp",
            self.partner,
        ).wait_recv()

    def start(self, piece):
        for copy in self.own_sends(piece):
            copy.start()

    def relay(self):
        for piece in range(self.pieces):
            for offset in range(1, self.nx):
                self.arrived(self.along_x(self.nx - offset, self.core), piece)
                self.forward(offset, piece).start()

    def finish(self):
        for piece in range(self.pieces):
            for offset in range(self.nx):
                self.arrived(self.along_x(offset, 1 - self.core), piece)
        for piece in range(self.pieces):
            for copy in self.own_sends(piece):
                copy.wait_send()
            for offset in range(1, self.nx):
                self.forward(offset, piece).wait_send()


def greet_tp(ntp, barrier):
    t = lax.axis_index("tp")
    for offset in range(1, ntp):
        pl.semaphore_signal(
            barrier, inc=1, device_id={"tp": lax.rem(t + offset, ntp)}, device_id_type=MESH
        )


def entry_kernel(
    nfs, ntp, ny, pieces,
    gate, up, down, tok, gains,
    gate_out, up_out, down_out, tok_out, gains_out,
    own_sem, send_sem, recv_sem, tok_own, tok_send, tok_fwd, tok_recv,
    gain_own, gain_send, gain_fwd, gain_recv,
):
    nz = nfs // ny
    f = lax.axis_index("fs")
    z, y = lax.div(f, ny), lax.rem(f, ny)
    barrier = pltpu.get_barrier_semaphore()
    greet_tp(ntp, barrier)
    for offset in range(1, ny):
        other = z * ny + lax.rem(y + offset, ny)
        pl.semaphore_signal(barrier, inc=1, device_id={"fs": other}, device_id_type=MESH)

    @pl.when(z > 0)
    def _():
        pl.semaphore_signal(barrier, inc=1, device_id={"fs": f - ny}, device_id_type=MESH)

    @pl.when(z < nz - 1)
    def _():
        pl.semaphore_signal(barrier, inc=1, device_id={"fs": f + ny}, device_id_type=MESH)

    ends = (z > 0).astype(jnp.int32) + (z < nz - 1).astype(jnp.int32)
    pl.semaphore_wait(barrier, ntp + ny - 2 + ends)

    shards = (gate, up, down)
    outs = (gate_out, up_out, down_out)

    def place(p, index):
        if p < 2:
            return outs[p].at[cols_at(index, shards[p].shape[0])]
        return outs[p].at[:, cols_at(index, shards[p].shape[1])]

    def along_z(p, step, zs, own):
        index = zs * ny + y
        block = place(p, index)
        kind = 0 if step > 0 else 1
        return remote(
            shards[p] if own else block, block, send_sem.at[kind, zs, p],
            recv_sem.at[index, p], "fs", f + step * ny,
        )

    def along_y(p, offset, zs, own):
        index = zs * ny + y
        block = place(p, index)
        return remote(
            shards[p] if own else block, block, send_sem.at[1 + offset, zs, p],
            recv_sem.at[index, p], "fs", z * ny + lax.rem(y + offset, ny),
        )

    def arrived(p, index):
        block = place(p, index)
        remote(block, block, send_sem.at[0, 0, p], recv_sem.at[index, p], "fs", f).wait_recv()

    toks = TpGather(ntp, tok, tok_out, tok_send, tok_fwd, tok_recv, pieces)
    gain = TpGather(ntp, gains, gains_out, gain_send, gain_fwd, gain_recv, 1)
    locals_ = [
        pltpu.make_async_copy(shards[p], place(p, f), own_sem.at[p]) for p in range(3)
    ]
    locals_.append(pltpu.make_async_copy(tok, tok_out.at[:, cols_at(toks.t, toks.width)], tok_own))
    locals_.append(
        pltpu.make_async_copy(gains, gains_out.at[:, cols_at(gain.t, gain.width)], gain_own)
    )

    def sends(zs, p, source_step, own, act):
        for step in (1, -1):
            if own or step == source_step:
                inside = (z < nz - 1) if step > 0 else (z > 0)

                @pl.when(inside)
                def _():
                    act(along_z(p, step, zs, own))

        for offset in range(1, ny):
            act(along_y(p, offset, zs, own))

    def all_z(act, wait):
        for distance in range(1, nz):
            for p in range(3):
                for step in (1, -1):
                    zs = z - step * distance

                    @pl.when(jnp.logical_and(zs >= 0, zs < nz))
                    def _():
                        if wait:
                            arrived(p, zs * ny + y)
                        sends(zs, p, step, False, act)

    for p in range(3):
        sends(z, p, 0, True, lambda copy: copy.start())
    gain.start(0)
    for piece in range(pieces):
        toks.start(piece)
    for copy in locals_:
        copy.start()
    gain.relay()
    toks.relay()
    all_z(lambda copy: copy.start(), True)
    for copy in locals_:
        copy.wait()
    gain.finish()
    toks.finish()
    for zs in range(nz):
        for p in range(3):
            for offset in range(1, ny):
                arrived(p, zs * ny + lax.rem(y + offset, ny))
    for p in range(3):
        sends(z, p, 0, True, lambda copy: copy.wait_send())
    all_z(lambda copy: copy.wait_send(), False)


def reduce_kernel(
    ntp, pieces, factor, gather,
    part, res, scale, *refs,
):
    if gather:
        (out, full, one, pair, two, s1, v1, s2, v2, own_sem, g_send, g_fwd, g_recv) = refs
    else:
        (out, one, pair, two, s1, v1, s2, v2) = refs
    t = lax.axis_index("tp")
    nx = ntp // 2
    core, chip = lax.rem(t, 2), lax.div(t, 2)
    partner = chip * 2 + (1 - core)
    width = res.shape[1]
    rows = res.shape[0] // pieces

    def at(piece):
        return pl.ds(piece * rows, rows)

    def along_x(offset, which):
        return lax.rem(chip + offset, nx) * 2 + which

    def to_partner(offset, piece):
        return remote(
            part.at[at(piece), cols_at(along_x(offset, 1 - core), width)],
            one.at[offset, at(piece)],
            s1.at[offset, piece], v1.at[offset, piece], "tp", partner,
        )

    def across(offset, piece):
        return remote(
            pair.at[offset - 1, at(piece)],
            two.at[offset - 1, at(piece)],
            s2.at[offset - 1, piece], v2.at[offset - 1, piece], "tp", along_x(offset, core),
        )

    barrier = pltpu.get_barrier_semaphore()
    greet_tp(ntp, barrier)
    pl.semaphore_wait(barrier, ntp - 1)
    for piece in range(pieces):
        for offset in range(1, nx):
            to_partner(offset, piece).start()
    for piece in range(pieces):
        to_partner(0, piece).start()
    for piece in range(pieces):
        for offset in range(1, nx):
            to_partner(offset, piece).wait_recv()
            mine = part[at(piece), cols_at(along_x(offset, core), width)].astype(F32)
            total = mine + one[offset, at(piece)].astype(F32)
            pair[offset - 1, at(piece)] = total.astype(BF16)
            across(offset, piece).start()
    if gather:
        spread = TpGather(ntp, out, full, g_send, g_fwd, g_recv, pieces)
    for piece in range(pieces):
        to_partner(0, piece).wait_recv()
        total = part[at(piece), cols_at(t, width)].astype(F32) + one[0, at(piece)].astype(F32)
        for offset in range(1, nx):
            across(offset, piece).wait_recv()
            total = total + two[offset - 1, at(piece)].astype(F32)
        value = res[at(piece)].astype(F32) + factor * total * scale[...]
        out[at(piece)] = value.astype(BF16)
        if gather:
            spread.start(piece)
    if gather:
        own = pltpu.make_async_copy(out, full.at[:, cols_at(t, width)], own_sem)
        own.start()
        spread.relay()
        spread.finish()
        own.wait()
    for piece in range(pieces):
        for offset in range(nx):
            to_partner(offset, piece).wait_send()
        for offset in range(1, nx):
            across(offset, piece).wait_send()


def retain_kernel(rate, query, key, value, outgate, cosines, sines, gain, out):
    length, width = query.shape
    even = lax.rem(lax.broadcasted_iota(jnp.int32, (length, width), 1), 2) == 0

    def turned(ref):
        v = ref[...].astype(F32)
        swapped = jnp.where(even, -pltpu.roll(v, width - 1, 1), pltpu.roll(v, 1, 1))
        return v * cosines[...] + swapped * sines[...]

    q = turned(query).astype(BF16)
    k = (turned(key) * width ** -0.5).astype(BF16)
    scores = lax.dot_general(q, k, (((1,), (1,)), ((), ())), preferred_element_type=F32)
    distance = lax.broadcasted_iota(jnp.int32, (length, length), 0) - lax.broadcasted_iota(
        jnp.int32, (length, length), 1
    )
    decay = jnp.exp(-rate[pl.program_id(0), 0] * jnp.maximum(distance, 0).astype(F32))
    scores = jnp.where(distance >= 0, scores * decay, 0.0).astype(BF16)
    kept = jnp.dot(scores, value[...], preferred_element_type=F32)
    kept = kept * lax.rsqrt(jnp.mean(kept * kept, axis=1, keepdims=True) + HEAD_EPS)
    g = outgate[...].astype(F32)
    out[...] = (kept * gain[...] * (g / (1.0 + jnp.exp(-g)))).astype(BF16)


def vmem():
    return pl.BlockSpec(memory_space=pltpu.VMEM)


def anywhere():
    return pl.BlockSpec(memory_space=pl.ANY)


def dma(*shape):
    return pltpu.SemaphoreType.DMA(shape)


def cost(flops):
    return pl.CostEstimate(flops=flops, bytes_accessed=2**20, transcendentals=0)


def enter(nfs, ntp, gate, up, down, tok, gains):
    ny = ntp // 2 if nfs % (ntp // 2) == 0 else 1
    nz, nx = nfs // ny, ntp // 2
    pieces = tok.shape[0] // LEN
    shape = jax.ShapeDtypeStruct
    return pl.pallas_call(
        functools.partial(entry_kernel, nfs, ntp, ny, pieces),
        out_shape=(
            shape((gate.shape[0] * nfs, gate.shape[1]), BF16),
            shape((up.shape[0] * nfs, up.shape[1]), BF16),
            shape((down.shape[0], down.shape[1] * nfs), BF16),
            shape((tok.shape[0], tok.shape[1] * ntp), BF16),
            shape((gains.shape[0], gains.shape[1] * ntp), F32),
        ),
        in_specs=[vmem()] * 5,
        out_specs=(anywhere(),) * 5,
        scratch_shapes=[
            dma(3), dma(ny + 1, nz, 3), dma(nfs, 3),
            dma(), dma(nx, pieces), dma(nx, pieces), dma(ntp, pieces),
            dma(), dma(nx, 1), dma(nx, 1), dma(ntp, 1),
        ],
        compiler_params=pltpu.CompilerParams(collective_id=0, has_side_effects=True),
        cost_estimate=cost(10**11),
        name="enter",
    )(gate, up, down, tok, gains)


def combine(ntp, identity, factor, gather, part, res, scale):
    pieces = res.shape[0] // LEN
    nx = ntp // 2
    rows, width = res.shape
    shape = jax.ShapeDtypeStruct
    out_shape = [shape((rows, width), BF16)]
    out_specs = [vmem()]
    scratch = [
        pltpu.VMEM((nx, rows, width), BF16),
        pltpu.VMEM((max(nx - 1, 1), rows, width), BF16),
        pltpu.VMEM((max(nx - 1, 1), rows, width), BF16),
        dma(nx, pieces), dma(nx, pieces),
        dma(max(nx - 1, 1), pieces), dma(max(nx - 1, 1), pieces),
    ]
    if gather:
        out_shape.append(shape((rows, width * ntp), BF16))
        out_specs.append(anywhere())
        scratch += [dma(), dma(nx, pieces), dma(nx, pieces), dma(ntp, pieces)]
    return pl.pallas_call(
        functools.partial(reduce_kernel, ntp, pieces, factor, gather),
        out_shape=tuple(out_shape),
        in_specs=[vmem()] * 3,
        out_specs=tuple(out_specs),
        scratch_shapes=scratch,
        compiler_params=pltpu.CompilerParams(collective_id=identity, has_side_effects=True),
        cost_estimate=cost(4 * 10**10),
        name="combine",
    )(part, res, scale)


def tables(length, width):
    freq = np.float32(1.0) / np.float32(10000.0) ** np.linspace(0.0, 1.0, width // 2, dtype=np.float32)
    angles = np.arange(length, dtype=np.float32)[:, None] * np.repeat(freq, 2)[None, :]
    return jnp.asarray(np.cos(angles)), jnp.asarray(np.sin(angles))


def retain(query, key, value, outgate, decay_rate, ret_gain):
    heads = decay_rate.shape[0]
    width = query.shape[1] // heads
    cosines, sines = tables(LEN, width)
    block = pl.BlockSpec((LEN, width), lambda h, s: (s, h))
    whole = pl.BlockSpec((LEN, width), lambda h, s: (0, 0))
    return pl.pallas_call(
        retain_kernel,
        grid=(heads, query.shape[0] // LEN),
        out_shape=jax.ShapeDtypeStruct(query.shape, BF16),
        in_specs=[
            pl.BlockSpec(memory_space=pltpu.SMEM), block, block, block, block, whole, whole,
            pl.BlockSpec((1, width), lambda h, s: (0, h)),
        ],
        out_specs=block,
        cost_estimate=cost(10**10),
        name="retain",
    )(decay_rate[:, None], query, key, value, outgate, cosines, sines, ret_gain[None])


def normed(full, gain):
    widened = full.astype(F32)
    mean = jnp.mean(widened * widened, axis=1, keepdims=True)
    return (widened * lax.rsqrt(mean + EPS) * gain).astype(BF16)


def dot(left, right):
    return jnp.dot(left, right, preferred_element_type=F32)


def ffn_part(features, gate, up, down, scale_gate, scale_up):
    hidden = jax.nn.silu(dot(features, gate) * scale_gate) * (dot(features, up) * scale_up)
    return dot(hidden.astype(BF16), down).astype(BF16)


def per_device(
    nfs, ntp,
    tokens, gain_one, w_gate, w_up, w_down, scale_gate, scale_up, scale_down,
    gain_mix, w_query, w_key, w_value, w_outgate,
    scale_query, scale_key, scale_value, scale_outgate,
    ret_gain, decay_rate, w_mix, scale_mix, gain_two,
):
    def gathered(weight, axis):
        return lax.all_gather(weight.astype(BF16), "fs", axis=axis, tiled=True)

    weights = [gathered(w, 0) for w in (w_query, w_key, w_value, w_outgate)]
    mix = gathered(w_mix, 1)
    gains = jnp.pad(jnp.stack((gain_one, gain_mix, gain_two)), ((0, 5), (0, 0)))
    gate, up, down, full, gains = enter(
        nfs, ntp, w_gate.astype(BF16), w_up.astype(BF16), w_down.astype(BF16), tokens, gains
    )
    part = ffn_part(normed(full, gains[0]), gate, up, down, scale_gate, scale_up)
    first, full = combine(ntp, 1, 0.5, True, part, tokens, scale_down[None])
    features = normed(full, gains[1])
    scales = (scale_query, scale_key, scale_value, scale_outgate)
    rows = [(dot(features, w) * s).astype(BF16) for w, s in zip(weights, scales)]
    mixed = retain(*rows, decay_rate, ret_gain)
    part = dot(mixed, mix).astype(BF16)
    second, full = combine(ntp, 2, 1.0, True, part, first, scale_mix[None])
    part = ffn_part(normed(full, gains[2]), gate, up, down, scale_gate, scale_up)
    return combine(ntp, 3, 0.5, False, part, second, scale_down[None])[0]


def solution(mesh):
    return jax.shard_map(
        functools.partial(per_device, mesh.shape["fs"], mesh.shape["tp"]),
        mesh=mesh,
        in_specs=(
            P("fs", "tp"),
            P("tp"),
            P("fs", "tp"),
            P("fs", "tp"),
            P("tp", "fs"),
            P("tp"),
            P("tp"),
            P("tp"),
            P("tp"),
            P("fs", "tp"),
            P("fs", "tp"),
            P("fs", "tp"),
            P("fs", "tp"),
            P("tp"),
            P("tp"),
            P("tp"),
            P("tp"),
            P("tp"),
            P("tp"),
            P("tp", "fs"),
            P("tp"),
            P("tp"),
        ),
        out_specs=P("fs", "tp"),
        check_vma=False,
    )
```

```python
import functools

import jax
import jax.numpy as jnp
import numpy as np
from jax import lax
from jax.experimental import pallas as pl
from jax.experimental.pallas import tpu as pltpu
from jax.sharding import PartitionSpec as P

LEN = 256
EPS = 1e-06
HEAD_EPS = 0.1
MESH = pl.DeviceIdType.MESH
BF16 = jnp.bfloat16
F32 = jnp.float32


def rows_of(ref, piece, rows):
    return ref.at[pl.ds(piece * rows, rows)]


def cols_at(index, width):
    return pl.ds(pl.multiple_of(index * width, width), width)


def remote(src, dst, send_sem, recv_sem, axis, target):
    return pltpu.make_async_remote_copy(
        src_ref=src,
        dst_ref=dst,
        send_sem=send_sem,
        recv_sem=recv_sem,
        device_id={axis: target},
        device_id_type=MESH,
    )


class TpGather:
    def __init__(self, ntp, src, out, sends, forwards, recvs, pieces):
        self.t = lax.axis_index("tp")
        self.nx = ntp // 2
        self.core = lax.rem(self.t, 2)
        self.chip = lax.div(self.t, 2)
        self.partner = self.chip * 2 + (1 - self.core)
        self.src, self.out = src, out
        self.sends, self.forwards, self.recvs = sends, forwards, recvs
        self.pieces = pieces
        self.rows = src.shape[0] // pieces
        self.width = src.shape[1]

    def along_x(self, offset, core):
        return lax.rem(self.chip + offset, self.nx) * 2 + core

    def place(self, index, piece):
        return self.out.at[pl.ds(piece * self.rows, self.rows), cols_at(index, self.width)]

    def own_sends(self, piece):
        src = rows_of(self.src, piece, self.rows)
        copies = []
        for offset in range(self.nx - 1, -1, -1):
            target = self.along_x(offset, self.core) if offset else self.partner
            copies.append(
                remote(
                    src,
                    self.place(self.t, piece),
                    self.sends.at[offset, piece],
                    self.recvs.at[self.t, piece],
                    "tp",
                    target,
                )
            )
        return copies

    def forward(self, offset, piece):
        index = self.along_x(self.nx - offset, self.core)
        block = self.place(index, piece)
        return remote(
            block,
            block,
            self.forwards.at[offset, piece],
            self.recvs.at[index, piece],
            "tp",
            self.partner,
        )

    def arrived(self, index, piece):
        block = self.place(index, piece)
        remote(
            block,
            block,
            self.sends.at[0, piece],
            self.recvs.at[index, piece],
            "tp",
            self.partner,
        ).wait_recv()

    def start(self, piece):
        for copy in self.own_sends(piece):
            copy.start()

    def relay(self):
        for piece in range(self.pieces):
            for offset in range(1, self.nx):
                self.arrived(self.along_x(self.nx - offset, self.core), piece)
                self.forward(offset, piece).start()

    def finish(self):
        for piece in range(self.pieces):
            for offset in range(self.nx):
                self.arrived(self.along_x(offset, 1 - self.core), piece)
        for piece in range(self.pieces):
            for copy in self.own_sends(piece):
                copy.wait_send()
            for offset in range(1, self.nx):
                self.forward(offset, piece).wait_send()


class FsGather:
    def __init__(self, nfs, ny, pieces, sends, recvs):
        self.ny, self.nz = ny, nfs // ny
        self.f = lax.axis_index("fs")
        self.z, self.y = lax.div(self.f, ny), lax.rem(self.f, ny)
        self.pieces = pieces
        self.sends, self.recvs = sends, recvs

    def source(self, p):
        src, _, _, part, parts, _ = self.pieces[p]
        step = src.shape[0] // parts
        return src.at[pl.ds(part * step, step)]

    def place(self, p, index):
        src, out, dim, part, parts, _ = self.pieces[p]
        rows, cols = src.shape
        step = rows // parts
        if dim == 0:
            return out.at[pl.ds(pl.multiple_of(index * rows + part * step, step), step)]
        return out.at[pl.ds(part * step, step), cols_at(index, cols)]

    def move(self, p, kind, index, own, target):
        block = self.place(p, index)
        return remote(
            self.source(p) if own else block, block,
            self.sends.at[kind, index, p], self.recvs.at[index, p], "fs", target,
        )

    def arrived(self, p, index):
        self.move(p, 0, index, False, self.f).wait_recv()

    def along_z(self, p, step, index, own, act):
        inside = (self.z < self.nz - 1) if step > 0 else (self.z > 0)

        @pl.when(inside)
        def _():
            act(self.move(p, 0 if step > 0 else 1, index, own, self.f + step * self.ny))

    def along_y(self, p, index, own, act):
        for offset in range(1, self.ny):
            target = self.z * self.ny + lax.rem(self.y + offset, self.ny)
            act(self.move(p, 1 + offset, index, own, target))

    def others(self, zs):
        return [zs * self.ny + lax.rem(self.y + offset, self.ny) for offset in range(1, self.ny)]

    def own(self, act, wait):
        order = range(len(self.pieces))
        for p in order:
            self.along_y(p, self.f, True, act)
            for step in (1, -1):
                self.along_z(p, step, self.f, True, act)
        for p in order:
            if self.pieces[p][5]:
                for index in self.others(self.z):
                    if wait:
                        self.arrived(p, index)
                    for step in (1, -1):
                        self.along_z(p, step, index, False, act)

    def relay(self, distance, act, wait):
        for p in range(len(self.pieces)):
            for step in (1, -1):
                zs = self.z - step * distance

                @pl.when(jnp.logical_and(zs >= 0, zs < self.nz))
                def _():
                    index = zs * self.ny + self.y
                    if wait:
                        self.arrived(p, index)
                    self.along_z(p, step, index, False, act)
                    if not self.pieces[p][5]:
                        self.along_y(p, index, False, act)

        for p in range(len(self.pieces)):
            if self.pieces[p][5]:
                for step in (1, -1):
                    zs = self.z - step * distance

                    @pl.when(jnp.logical_and(zs >= 0, zs < self.nz))
                    def _():
                        for index in self.others(zs):
                            if wait:
                                self.arrived(p, index)
                            self.along_z(p, step, index, False, act)

    def start_own(self):
        self.own(lambda copy: copy.start(), True)

    def start_relay(self, distance):
        self.relay(distance, lambda copy: copy.start(), True)

    def finish(self):
        for p in range(len(self.pieces)):
            if not self.pieces[p][5]:
                for zs in range(self.nz):
                    for index in self.others(zs):
                        self.arrived(p, index)
        self.own(lambda copy: copy.wait_send(), False)
        for distance in range(1, self.nz):
            self.relay(distance, lambda copy: copy.wait_send(), False)

    def greet(self, barrier):
        ny, z, f = self.ny, self.z, self.f
        for index in self.others(z):
            pl.semaphore_signal(barrier, inc=1, device_id={"fs": index}, device_id_type=MESH)

        @pl.when(z > 0)
        def _():
            pl.semaphore_signal(barrier, inc=1, device_id={"fs": f - ny}, device_id_type=MESH)

        @pl.when(z < self.nz - 1)
        def _():
            pl.semaphore_signal(barrier, inc=1, device_id={"fs": f + ny}, device_id_type=MESH)

        ends = (z > 0).astype(jnp.int32) + (z < self.nz - 1).astype(jnp.int32)
        return ends + (ny - 1)

    def own_copies(self, sems):
        return [
            pltpu.make_async_copy(self.source(p), self.place(p, self.f), sems.at[p])
            for p in range(len(self.pieces))
        ]


def greet_tp(ntp, barrier):
    t = lax.axis_index("tp")
    for offset in range(1, ntp):
        pl.semaphore_signal(
            barrier, inc=1, device_id={"tp": lax.rem(t + offset, ntp)}, device_id_type=MESH
        )


def entry_kernel(
    nfs, ntp, ny, pieces,
    gate, up, down, tok, gains,
    gate_out, up_out, down_out, tok_out, gains_out,
    own_sem, send_sem, recv_sem, tok_own, tok_send, tok_fwd, tok_recv,
    gain_own, gain_send, gain_fwd, gain_recv,
):
    shards = ((gate, gate_out, 0), (up, up_out, 0), (down, down_out, 1))
    parts = [(*shard, half, 2, i == 0 and half == 0) for i, shard in enumerate(shards) for half in range(2)]
    weights = FsGather(nfs, ny, parts, send_sem, recv_sem)
    barrier = pltpu.get_barrier_semaphore()
    greet_tp(ntp, barrier)
    pl.semaphore_wait(barrier, weights.greet(barrier) + (ntp - 1))
    toks = TpGather(ntp, tok, tok_out, tok_send, tok_fwd, tok_recv, pieces)
    gain = TpGather(ntp, gains, gains_out, gain_send, gain_fwd, gain_recv, 1)
    copies = weights.own_copies(own_sem)
    copies.append(pltpu.make_async_copy(tok, tok_out.at[:, cols_at(toks.t, toks.width)], tok_own))
    copies.append(
        pltpu.make_async_copy(gains, gains_out.at[:, cols_at(gain.t, gain.width)], gain_own)
    )
    gain.start(0)
    for piece in range(pieces):
        toks.start(piece)
    weights.start_own()
    for copy in copies:
        copy.start()
    for distance in range(1, weights.nz):
        weights.start_relay(distance)
        if distance == 1:
            gain.relay()
            toks.relay()
    for copy in copies:
        copy.wait()
    gain.finish()
    toks.finish()
    weights.finish()


def reduce_kernel(
    nfs, ntp, ny, pieces, factor, gather, dims,
    part, res, scale, *refs,
):
    count = len(dims)
    shards, refs = refs[:count], refs[count:]
    if count:
        wholes = refs[2 : 2 + count]
        refs, (w_own, w_send, w_recv) = refs[:2] + refs[2 + count : -3], refs[-3:]
    if gather:
        (out, full, one, pair, two, s1, v1, s2, v2, own_sem, g_send, g_fwd, g_recv) = refs
    else:
        (out, one, pair, two, s1, v1, s2, v2) = refs
    t = lax.axis_index("tp")
    nx = ntp // 2
    core, chip = lax.rem(t, 2), lax.div(t, 2)
    partner = chip * 2 + (1 - core)
    width = res.shape[1]
    rows = res.shape[0] // pieces

    def at(piece):
        return pl.ds(piece * rows, rows)

    def along_x(offset, which):
        return lax.rem(chip + offset, nx) * 2 + which

    def to_partner(offset, piece):
        return remote(
            part.at[at(piece), cols_at(along_x(offset, 1 - core), width)],
            one.at[offset, at(piece)],
            s1.at[offset, piece], v1.at[offset, piece], "tp", partner,
        )

    def across(offset, piece):
        return remote(
            pair.at[offset - 1, at(piece)],
            two.at[offset - 1, at(piece)],
            s2.at[offset - 1, piece], v2.at[offset - 1, piece], "tp", along_x(offset, core),
        )

    barrier = pltpu.get_barrier_semaphore()
    greet_tp(ntp, barrier)
    if count:
        parts = [(shards[i], wholes[i], dims[i], 0, 1, i == 0) for i in range(count)]
        weights = FsGather(nfs, ny, parts, w_send, w_recv)
        pl.semaphore_wait(barrier, weights.greet(barrier) + (ntp - 1))
    else:
        pl.semaphore_wait(barrier, ntp - 1)
    for piece in range(pieces):
        for offset in range(1, nx):
            to_partner(offset, piece).start()
    for piece in range(pieces):
        to_partner(0, piece).start()
    if count:
        weights.start_own()
        copies = weights.own_copies(w_own)
        for copy in copies:
            copy.start()
    for piece in range(pieces):
        for offset in range(1, nx):
            to_partner(offset, piece).wait_recv()
            mine = part[at(piece), cols_at(along_x(offset, core), width)].astype(F32)
            total = mine + one[offset, at(piece)].astype(F32)
            pair[offset - 1, at(piece)] = total.astype(BF16)
            across(offset, piece).start()
    if gather:
        spread = TpGather(ntp, out, full, g_send, g_fwd, g_recv, pieces)
    for piece in range(pieces):
        to_partner(0, piece).wait_recv()
        total = part[at(piece), cols_at(t, width)].astype(F32) + one[0, at(piece)].astype(F32)
        for offset in range(1, nx):
            across(offset, piece).wait_recv()
            total = total + two[offset - 1, at(piece)].astype(F32)
        value = res[at(piece)].astype(F32) + factor * total * scale[...]
        out[at(piece)] = value.astype(BF16)
        if gather:
            spread.start(piece)
    if gather:
        own = pltpu.make_async_copy(out, full.at[:, cols_at(t, width)], own_sem)
        own.start()
        if count:
            weights.start_relay(1)
        spread.relay()
        if count:
            for distance in range(2, weights.nz):
                weights.start_relay(distance)
        spread.finish()
        own.wait()
    if count:
        for copy in copies:
            copy.wait()
        weights.finish()
    for piece in range(pieces):
        for offset in range(nx):
            to_partner(offset, piece).wait_send()
        for offset in range(1, nx):
            across(offset, piece).wait_send()


def retain_kernel(rate, query, key, value, outgate, cosines, sines, gain, out):
    length, width = query.shape
    even = lax.rem(lax.broadcasted_iota(jnp.int32, (length, width), 1), 2) == 0

    def turned(ref):
        v = ref[...].astype(F32)
        swapped = jnp.where(even, -pltpu.roll(v, width - 1, 1), pltpu.roll(v, 1, 1))
        return v * cosines[...] + swapped * sines[...]

    q = turned(query).astype(BF16)
    k = (turned(key) * width ** -0.5).astype(BF16)
    scores = lax.dot_general(q, k, (((1,), (1,)), ((), ())), preferred_element_type=F32)
    distance = lax.broadcasted_iota(jnp.int32, (length, length), 0) - lax.broadcasted_iota(
        jnp.int32, (length, length), 1
    )
    decay = jnp.exp(-rate[pl.program_id(0), 0] * jnp.maximum(distance, 0).astype(F32))
    scores = jnp.where(distance >= 0, scores * decay, 0.0).astype(BF16)
    kept = jnp.dot(scores, value[...], preferred_element_type=F32)
    kept = kept * lax.rsqrt(jnp.mean(kept * kept, axis=1, keepdims=True) + HEAD_EPS)
    g = outgate[...].astype(F32)
    out[...] = (kept * gain[...] * (g / (1.0 + jnp.exp(-g)))).astype(BF16)


def vmem():
    return pl.BlockSpec(memory_space=pltpu.VMEM)


def anywhere():
    return pl.BlockSpec(memory_space=pl.ANY)


def dma(*shape):
    return pltpu.SemaphoreType.DMA(shape)


def cost(flops):
    return pl.CostEstimate(flops=flops, bytes_accessed=2**20, transcendentals=0)


def along_y_of(nfs, ntp):
    return ntp // 2 if nfs % (ntp // 2) == 0 else 1


def enter(nfs, ntp, gate, up, down, tok, gains):
    ny, nx = along_y_of(nfs, ntp), ntp // 2
    pieces = tok.shape[0] // LEN
    shape = jax.ShapeDtypeStruct
    return pl.pallas_call(
        functools.partial(entry_kernel, nfs, ntp, ny, pieces),
        out_shape=(
            shape((gate.shape[0] * nfs, gate.shape[1]), BF16),
            shape((up.shape[0] * nfs, up.shape[1]), BF16),
            shape((down.shape[0], down.shape[1] * nfs), BF16),
            shape((tok.shape[0], tok.shape[1] * ntp), BF16),
            shape((gains.shape[0], gains.shape[1] * ntp), F32),
        ),
        in_specs=[vmem()] * 5,
        out_specs=(anywhere(),) * 5,
        scratch_shapes=[
            dma(6), dma(ny + 1, nfs, 6), dma(nfs, 6),
            dma(), dma(nx, pieces), dma(nx, pieces), dma(ntp, pieces),
            dma(), dma(nx, 1), dma(nx, 1), dma(ntp, 1),
        ],
        compiler_params=pltpu.CompilerParams(collective_id=0, has_side_effects=True),
        cost_estimate=cost(10**11),
        name="enter",
    )(gate, up, down, tok, gains)


def combine(nfs, ntp, identity, factor, gather, part, res, scale, shards=(), dims=()):
    ny, count = along_y_of(nfs, ntp), len(dims)
    pieces = res.shape[0] // LEN
    nx = ntp // 2
    rows, width = res.shape
    shape = jax.ShapeDtypeStruct
    out_shape = [shape((rows, width), BF16)]
    out_specs = [vmem()]
    scratch = [
        pltpu.VMEM((nx, rows, width), BF16),
        pltpu.VMEM((max(nx - 1, 1), rows, width), BF16),
        pltpu.VMEM((max(nx - 1, 1), rows, width), BF16),
        dma(nx, pieces), dma(nx, pieces),
        dma(max(nx - 1, 1), pieces), dma(max(nx - 1, 1), pieces),
    ]
    if gather:
        out_shape.append(shape((rows, width * ntp), BF16))
        out_specs.append(anywhere())
        scratch += [dma(), dma(nx, pieces), dma(nx, pieces), dma(ntp, pieces)]
    if count:
        for shard, dim in zip(shards, dims):
            grown = [size * (nfs if axis == dim else 1) for axis, size in enumerate(shard.shape)]
            out_shape.append(shape(tuple(grown), BF16))
            out_specs.append(anywhere())
        scratch += [dma(count), dma(ny + 1, nfs, count), dma(nfs, count)]
    return pl.pallas_call(
        functools.partial(reduce_kernel, nfs, ntp, ny, pieces, factor, gather, dims),
        out_shape=tuple(out_shape),
        in_specs=[vmem()] * (3 + count),
        out_specs=tuple(out_specs),
        scratch_shapes=scratch,
        compiler_params=pltpu.CompilerParams(collective_id=identity, has_side_effects=True),
        cost_estimate=cost(4 * 10**10),
        name="combine",
    )(part, res, scale, *shards)


def tables(length, width):
    freq = np.float32(1.0) / np.float32(10000.0) ** np.linspace(0.0, 1.0, width // 2, dtype=np.float32)
    angles = np.arange(length, dtype=np.float32)[:, None] * np.repeat(freq, 2)[None, :]
    return jnp.asarray(np.cos(angles)), jnp.asarray(np.sin(angles))


def retain(query, key, value, outgate, decay_rate, ret_gain):
    heads = decay_rate.shape[0]
    width = query.shape[1] // heads
    cosines, sines = tables(LEN, width)
    block = pl.BlockSpec((LEN, width), lambda h, s: (s, h))
    whole = pl.BlockSpec((LEN, width), lambda h, s: (0, 0))
    return pl.pallas_call(
        retain_kernel,
        grid=(heads, query.shape[0] // LEN),
        out_shape=jax.ShapeDtypeStruct(query.shape, BF16),
        in_specs=[
            pl.BlockSpec(memory_space=pltpu.SMEM), block, block, block, block, whole, whole,
            pl.BlockSpec((1, width), lambda h, s: (0, h)),
        ],
        out_specs=block,
        cost_estimate=cost(10**10),
        name="retain",
    )(decay_rate[:, None], query, key, value, outgate, cosines, sines, ret_gain[None])


def normed(full, gain):
    widened = full.astype(F32)
    mean = jnp.mean(widened * widened, axis=1, keepdims=True)
    return (widened * lax.rsqrt(mean + EPS) * gain).astype(BF16)


def dot(left, right):
    return jnp.dot(left, right, preferred_element_type=F32)


def ffn_part(features, gate, up, down, scale_gate, scale_up):
    hidden = jax.nn.silu(dot(features, gate) * scale_gate) * (dot(features, up) * scale_up)
    return dot(hidden.astype(BF16), down).astype(BF16)


def per_device(
    nfs, ntp,
    tokens, gain_one, w_gate, w_up, w_down, scale_gate, scale_up, scale_down,
    gain_mix, w_query, w_key, w_value, w_outgate,
    scale_query, scale_key, scale_value, scale_outgate,
    ret_gain, decay_rate, w_mix, scale_mix, gain_two,
):
    shards = [w.astype(BF16) for w in (w_query, w_key, w_value, w_outgate, w_mix)]
    gains = jnp.pad(jnp.stack((gain_one, gain_mix, gain_two)), ((0, 5), (0, 0)))
    gate, up, down, full, gains = enter(
        nfs, ntp, w_gate.astype(BF16), w_up.astype(BF16), w_down.astype(BF16), tokens, gains
    )
    part = ffn_part(normed(full, gains[0]), gate, up, down, scale_gate, scale_up)
    first, full, *weights, mix = combine(
        nfs, ntp, 1, 0.5, True, part, tokens, scale_down[None], shards, (0, 0, 0, 0, 1)
    )
    features = normed(full, gains[1])
    scales = (scale_query, scale_key, scale_value, scale_outgate)
    rows = [(dot(features, w) * s).astype(BF16) for w, s in zip(weights, scales)]
    mixed = retain(*rows, decay_rate, ret_gain)
    part = dot(mixed, mix).astype(BF16)
    second, full = combine(nfs, ntp, 2, 1.0, True, part, first, scale_mix[None])
    part = ffn_part(normed(full, gains[2]), gate, up, down, scale_gate, scale_up)
    return combine(nfs, ntp, 3, 0.5, False, part, second, scale_down[None])[0]


def solution(mesh):
    return jax.shard_map(
        functools.partial(per_device, mesh.shape["fs"], mesh.shape["tp"]),
        mesh=mesh,
        in_specs=(
            P("fs", "tp"),
            P("tp"),
            P("fs", "tp"),
            P("fs", "tp"),
            P("tp", "fs"),
            P("tp"),
            P("tp"),
            P("tp"),
            P("tp"),
            P("fs", "tp"),
            P("fs", "tp"),
            P("fs", "tp"),
            P("fs", "tp"),
            P("tp"),
            P("tp"),
            P("tp"),
            P("tp"),
            P("tp"),
            P("tp"),
            P("tp", "fs"),
            P("tp"),
            P("tp"),
        ),
        out_specs=P("fs", "tp"),
        check_vma=False,
    )
```

```python
import functools

import jax
import jax.numpy as jnp
import numpy as np
from jax import lax
from jax.experimental import pallas as pl
from jax.experimental.pallas import tpu as pltpu
from jax.sharding import PartitionSpec as P

LEN = 256
EPS = 1e-06
HEAD_EPS = 0.1
MESH = pl.DeviceIdType.MESH
BF16 = jnp.bfloat16
F32 = jnp.float32


def rows_of(ref, piece, rows):
    return ref.at[pl.ds(piece * rows, rows)]


def cols_at(index, width):
    return pl.ds(pl.multiple_of(index * width, width), width)


def remote(src, dst, send_sem, recv_sem, axis, target):
    return pltpu.make_async_remote_copy(
        src_ref=src,
        dst_ref=dst,
        send_sem=send_sem,
        recv_sem=recv_sem,
        device_id={axis: target},
        device_id_type=MESH,
    )


class TpGather:
    def __init__(self, ntp, src, out, sends, forwards, recvs, pieces):
        self.t = lax.axis_index("tp")
        self.nx = ntp // 2
        self.core = lax.rem(self.t, 2)
        self.chip = lax.div(self.t, 2)
        self.partner = self.chip * 2 + (1 - self.core)
        self.src, self.out = src, out
        self.sends, self.forwards, self.recvs = sends, forwards, recvs
        self.pieces = pieces
        self.rows = src.shape[0] // pieces
        self.width = src.shape[1]

    def along_x(self, offset, core):
        return lax.rem(self.chip + offset, self.nx) * 2 + core

    def place(self, index, piece):
        return self.out.at[pl.ds(piece * self.rows, self.rows), cols_at(index, self.width)]

    def own_sends(self, piece):
        src = rows_of(self.src, piece, self.rows)
        copies = []
        for offset in range(self.nx - 1, -1, -1):
            target = self.along_x(offset, self.core) if offset else self.partner
            copies.append(
                remote(
                    src,
                    self.place(self.t, piece),
                    self.sends.at[offset, piece],
                    self.recvs.at[self.t, piece],
                    "tp",
                    target,
                )
            )
        return copies

    def forward(self, offset, piece):
        index = self.along_x(self.nx - offset, self.core)
        block = self.place(index, piece)
        return remote(
            block,
            block,
            self.forwards.at[offset, piece],
            self.recvs.at[index, piece],
            "tp",
            self.partner,
        )

    def arrived(self, index, piece):
        block = self.place(index, piece)
        remote(
            block,
            block,
            self.sends.at[0, piece],
            self.recvs.at[index, piece],
            "tp",
            self.partner,
        ).wait_recv()

    def start(self, piece):
        for copy in self.own_sends(piece):
            copy.start()

    def relay(self):
        for piece in range(self.pieces):
            for offset in range(1, self.nx):
                self.arrived(self.along_x(self.nx - offset, self.core), piece)
                self.forward(offset, piece).start()

    def finish(self):
        for piece in range(self.pieces):
            for offset in range(self.nx):
                self.arrived(self.along_x(offset, 1 - self.core), piece)
        for piece in range(self.pieces):
            for copy in self.own_sends(piece):
                copy.wait_send()
            for offset in range(1, self.nx):
                self.forward(offset, piece).wait_send()


class FsGather:
    def __init__(self, nfs, ny, pieces, sends, recvs):
        self.ny, self.nz = ny, nfs // ny
        self.f = lax.axis_index("fs")
        self.z, self.y = lax.div(self.f, ny), lax.rem(self.f, ny)
        self.pieces = pieces
        self.sends, self.recvs = sends, recvs

    def source(self, p):
        src, _, _, part, parts, _ = self.pieces[p]
        step = src.shape[0] // parts
        return src.at[pl.ds(part * step, step)]

    def place(self, p, index):
        src, out, dim, part, parts, _ = self.pieces[p]
        rows, cols = src.shape
        step = rows // parts
        if dim == 0:
            return out.at[pl.ds(pl.multiple_of(index * rows + part * step, step), step)]
        return out.at[pl.ds(part * step, step), cols_at(index, cols)]

    def move(self, p, kind, index, own, target):
        block = self.place(p, index)
        return remote(
            self.source(p) if own else block, block,
            self.sends.at[kind, index, p], self.recvs.at[index, p], "fs", target,
        )

    def arrived(self, p, index):
        self.move(p, 0, index, False, self.f).wait_recv()

    def along_z(self, p, step, index, own, act):
        inside = (self.z < self.nz - 1) if step > 0 else (self.z > 0)

        @pl.when(inside)
        def _():
            act(self.move(p, 0 if step > 0 else 1, index, own, self.f + step * self.ny))

    def along_y(self, p, index, own, act):
        for offset in range(1, self.ny):
            target = self.z * self.ny + lax.rem(self.y + offset, self.ny)
            act(self.move(p, 1 + offset, index, own, target))

    def others(self, zs):
        return [zs * self.ny + lax.rem(self.y + offset, self.ny) for offset in range(1, self.ny)]

    def own(self, act, wait):
        order = range(len(self.pieces))
        for p in order:
            self.along_y(p, self.f, True, act)
            for step in (1, -1):
                self.along_z(p, step, self.f, True, act)
        for p in order:
            if self.pieces[p][5]:
                for index in self.others(self.z):
                    if wait:
                        self.arrived(p, index)
                    for step in (1, -1):
                        self.along_z(p, step, index, False, act)

    def relay(self, distance, act, wait):
        for p in range(len(self.pieces)):
            for step in (1, -1):
                zs = self.z - step * distance

                @pl.when(jnp.logical_and(zs >= 0, zs < self.nz))
                def _():
                    index = zs * self.ny + self.y
                    if wait:
                        self.arrived(p, index)
                    self.along_z(p, step, index, False, act)
                    if not self.pieces[p][5]:
                        self.along_y(p, index, False, act)

        for p in range(len(self.pieces)):
            if self.pieces[p][5]:
                for step in (1, -1):
                    zs = self.z - step * distance

                    @pl.when(jnp.logical_and(zs >= 0, zs < self.nz))
                    def _():
                        for index in self.others(zs):
                            if wait:
                                self.arrived(p, index)
                            self.along_z(p, step, index, False, act)

    def start_own(self):
        self.own(lambda copy: copy.start(), True)

    def start_relay(self, distance):
        self.relay(distance, lambda copy: copy.start(), True)

    def finish(self):
        for p in range(len(self.pieces)):
            if not self.pieces[p][5]:
                for zs in range(self.nz):
                    for index in self.others(zs):
                        self.arrived(p, index)
        self.own(lambda copy: copy.wait_send(), False)
        for distance in range(1, self.nz):
            self.relay(distance, lambda copy: copy.wait_send(), False)

    def greet(self, barrier):
        ny, z, f = self.ny, self.z, self.f
        for index in self.others(z):
            pl.semaphore_signal(barrier, inc=1, device_id={"fs": index}, device_id_type=MESH)

        @pl.when(z > 0)
        def _():
            pl.semaphore_signal(barrier, inc=1, device_id={"fs": f - ny}, device_id_type=MESH)

        @pl.when(z < self.nz - 1)
        def _():
            pl.semaphore_signal(barrier, inc=1, device_id={"fs": f + ny}, device_id_type=MESH)

        ends = (z > 0).astype(jnp.int32) + (z < self.nz - 1).astype(jnp.int32)
        return ends + (ny - 1)

    def own_copies(self, sems):
        return [
            pltpu.make_async_copy(self.source(p), self.place(p, self.f), sems.at[p])
            for p in range(len(self.pieces))
        ]


def greet_tp(ntp, barrier):
    t = lax.axis_index("tp")
    for offset in range(1, ntp):
        pl.semaphore_signal(
            barrier, inc=1, device_id={"tp": lax.rem(t + offset, ntp)}, device_id_type=MESH
        )


def entry_kernel(
    nfs, ntp, ny, pieces,
    gate, up, down, tok, gains,
    gate_out, up_out, down_out, tok_out, gains_out,
    own_sem, send_sem, recv_sem, tok_own, tok_send, tok_fwd, tok_recv,
    gain_own, gain_send, gain_fwd, gain_recv,
):
    shards = ((gate, gate_out, 0), (up, up_out, 0), (down, down_out, 1))
    parts = [(*shard, half, 2, i == 0 and half == 0) for i, shard in enumerate(shards) for half in range(2)]
    weights = FsGather(nfs, ny, parts, send_sem, recv_sem)
    barrier = pltpu.get_barrier_semaphore()
    greet_tp(ntp, barrier)
    pl.semaphore_wait(barrier, weights.greet(barrier) + (ntp - 1))
    toks = TpGather(ntp, tok, tok_out, tok_send, tok_fwd, tok_recv, pieces)
    gain = TpGather(ntp, gains, gains_out, gain_send, gain_fwd, gain_recv, 1)
    copies = weights.own_copies(own_sem)
    copies.append(pltpu.make_async_copy(tok, tok_out.at[:, cols_at(toks.t, toks.width)], tok_own))
    copies.append(
        pltpu.make_async_copy(gains, gains_out.at[:, cols_at(gain.t, gain.width)], gain_own)
    )
    gain.start(0)
    for piece in range(pieces):
        toks.start(piece)
    weights.start_own()
    for copy in copies:
        copy.start()
    for distance in range(1, weights.nz):
        weights.start_relay(distance)
        if distance == 1:
            gain.relay()
            toks.relay()
    for copy in copies:
        copy.wait()
    gain.finish()
    toks.finish()
    weights.finish()


def reduce_kernel(
    nfs, ntp, ny, pieces, factor, gather, dims,
    part, res, scale, *refs,
):
    count = len(dims)
    shards, refs = refs[:count], refs[count:]
    if count:
        wholes = refs[2 : 2 + count]
        refs, (w_own, w_send, w_recv) = refs[:2] + refs[2 + count : -3], refs[-3:]
    if gather:
        (out, full, one, pair, two, s1, v1, s2, v2, own_sem, g_send, g_fwd, g_recv) = refs
    else:
        (out, one, pair, two, s1, v1, s2, v2) = refs
    t = lax.axis_index("tp")
    nx = ntp // 2
    core, chip = lax.rem(t, 2), lax.div(t, 2)
    partner = chip * 2 + (1 - core)
    width = res.shape[1]
    rows = res.shape[0] // pieces

    def at(piece):
        return pl.ds(piece * rows, rows)

    def along_x(offset, which):
        return lax.rem(chip + offset, nx) * 2 + which

    def to_partner(offset, piece):
        return remote(
            part.at[at(piece), cols_at(along_x(offset, 1 - core), width)],
            one.at[offset, at(piece)],
            s1.at[offset, piece], v1.at[offset, piece], "tp", partner,
        )

    def across(offset, piece):
        return remote(
            pair.at[offset - 1, at(piece)],
            two.at[offset - 1, at(piece)],
            s2.at[offset - 1, piece], v2.at[offset - 1, piece], "tp", along_x(offset, core),
        )

    barrier = pltpu.get_barrier_semaphore()
    greet_tp(ntp, barrier)
    if count:
        parts = [(shards[i], wholes[i], dims[i], 0, 1, i == 0) for i in range(count)]
        weights = FsGather(nfs, ny, parts, w_send, w_recv)
        pl.semaphore_wait(barrier, weights.greet(barrier) + (ntp - 1))
    else:
        pl.semaphore_wait(barrier, ntp - 1)
    for piece in range(pieces):
        for offset in range(1, nx):
            to_partner(offset, piece).start()
    for piece in range(pieces):
        to_partner(0, piece).start()
    if count:
        weights.start_own()
        copies = weights.own_copies(w_own)
        for copy in copies:
            copy.start()
    for piece in range(pieces):
        for offset in range(1, nx):
            to_partner(offset, piece).wait_recv()
            mine = part[at(piece), cols_at(along_x(offset, core), width)].astype(F32)
            total = mine + one[offset, at(piece)].astype(F32)
            pair[offset - 1, at(piece)] = total.astype(BF16)
            across(offset, piece).start()
    if gather:
        spread = TpGather(ntp, out, full, g_send, g_fwd, g_recv, pieces)
    for piece in range(pieces):
        to_partner(0, piece).wait_recv()
        total = part[at(piece), cols_at(t, width)].astype(F32) + one[0, at(piece)].astype(F32)
        for offset in range(1, nx):
            across(offset, piece).wait_recv()
            total = total + two[offset - 1, at(piece)].astype(F32)
        value = res[at(piece)].astype(F32) + factor * total * scale[...]
        out[at(piece)] = value.astype(BF16)
        if gather:
            spread.start(piece)
    if gather:
        own = pltpu.make_async_copy(out, full.at[:, cols_at(t, width)], own_sem)
        own.start()
        if count:
            weights.start_relay(1)
        spread.relay()
        if count:
            for distance in range(2, weights.nz):
                weights.start_relay(distance)
        spread.finish()
        own.wait()
    if count:
        for copy in copies:
            copy.wait()
        weights.finish()
    for piece in range(pieces):
        for offset in range(nx):
            to_partner(offset, piece).wait_send()
        for offset in range(1, nx):
            across(offset, piece).wait_send()


def retain_kernel(rate, query, key, value, outgate, cosines, sines, gain, out):
    length, width = query.shape
    even = lax.rem(lax.broadcasted_iota(jnp.int32, (length, width), 1), 2) == 0

    def turned(ref):
        v = ref[...].astype(F32)
        swapped = jnp.where(even, -pltpu.roll(v, width - 1, 1), pltpu.roll(v, 1, 1))
        return v * cosines[...] + swapped * sines[...]

    q = turned(query).astype(BF16)
    k = (turned(key) * width ** -0.5).astype(BF16)
    scores = lax.dot_general(q, k, (((1,), (1,)), ((), ())), preferred_element_type=F32)
    distance = lax.broadcasted_iota(jnp.int32, (length, length), 0) - lax.broadcasted_iota(
        jnp.int32, (length, length), 1
    )
    decay = jnp.exp(-rate[pl.program_id(0), 0] * jnp.maximum(distance, 0).astype(F32))
    scores = jnp.where(distance >= 0, scores * decay, 0.0).astype(BF16)
    kept = jnp.dot(scores, value[...], preferred_element_type=F32)
    kept = kept * lax.rsqrt(jnp.mean(kept * kept, axis=1, keepdims=True) + HEAD_EPS)
    g = outgate[...].astype(F32)
    out[...] = (kept * gain[...] * (g / (1.0 + jnp.exp(-g)))).astype(BF16)


def vmem():
    return pl.BlockSpec(memory_space=pltpu.VMEM)


def anywhere():
    return pl.BlockSpec(memory_space=pl.ANY)


def dma(*shape):
    return pltpu.SemaphoreType.DMA(shape)


def cost(flops):
    return pl.CostEstimate(flops=flops, bytes_accessed=2**20, transcendentals=0)


def along_y_of(nfs, ntp):
    return ntp // 2 if nfs % (ntp // 2) == 0 else 1


def enter(nfs, ntp, gate, up, down, tok, gains):
    ny, nx = along_y_of(nfs, ntp), ntp // 2
    pieces = tok.shape[0] // LEN
    shape = jax.ShapeDtypeStruct
    return pl.pallas_call(
        functools.partial(entry_kernel, nfs, ntp, ny, pieces),
        out_shape=(
            shape((gate.shape[0] * nfs, gate.shape[1]), BF16),
            shape((up.shape[0] * nfs, up.shape[1]), BF16),
            shape((down.shape[0], down.shape[1] * nfs), BF16),
            shape((tok.shape[0], tok.shape[1] * ntp), BF16),
            shape((gains.shape[0], gains.shape[1] * ntp), F32),
        ),
        in_specs=[vmem()] * 5,
        out_specs=(anywhere(),) * 5,
        scratch_shapes=[
            dma(6), dma(ny + 1, nfs, 6), dma(nfs, 6),
            dma(), dma(nx, pieces), dma(nx, pieces), dma(ntp, pieces),
            dma(), dma(nx, 1), dma(nx, 1), dma(ntp, 1),
        ],
        compiler_params=pltpu.CompilerParams(collective_id=0, has_side_effects=True),
        cost_estimate=cost(10**11),
        name="enter",
    )(gate, up, down, tok, gains)


def combine(nfs, ntp, identity, factor, gather, part, res, scale, shards=(), dims=()):
    ny, count = along_y_of(nfs, ntp), len(dims)
    pieces = res.shape[0] // (LEN // 2)
    nx = ntp // 2
    rows, width = res.shape
    shape = jax.ShapeDtypeStruct
    out_shape = [shape((rows, width), BF16)]
    out_specs = [vmem()]
    scratch = [
        pltpu.VMEM((nx, rows, width), BF16),
        pltpu.VMEM((max(nx - 1, 1), rows, width), BF16),
        pltpu.VMEM((max(nx - 1, 1), rows, width), BF16),
        dma(nx, pieces), dma(nx, pieces),
        dma(max(nx - 1, 1), pieces), dma(max(nx - 1, 1), pieces),
    ]
    if gather:
        out_shape.append(shape((rows, width * ntp), BF16))
        out_specs.append(anywhere())
        scratch += [dma(), dma(nx, pieces), dma(nx, pieces), dma(ntp, pieces)]
    if count:
        for shard, dim in zip(shards, dims):
            grown = [size * (nfs if axis == dim else 1) for axis, size in enumerate(shard.shape)]
            out_shape.append(shape(tuple(grown), BF16))
            out_specs.append(anywhere())
        scratch += [dma(count), dma(ny + 1, nfs, count), dma(nfs, count)]
    return pl.pallas_call(
        functools.partial(reduce_kernel, nfs, ntp, ny, pieces, factor, gather, dims),
        out_shape=tuple(out_shape),
        in_specs=[vmem()] * (3 + count),
        out_specs=tuple(out_specs),
        scratch_shapes=scratch,
        compiler_params=pltpu.CompilerParams(collective_id=identity, has_side_effects=True),
        cost_estimate=cost(4 * 10**10),
        name="combine",
    )(part, res, scale, *shards)


def tables(length, width):
    freq = np.float32(1.0) / np.float32(10000.0) ** np.linspace(0.0, 1.0, width // 2, dtype=np.float32)
    angles = np.arange(length, dtype=np.float32)[:, None] * np.repeat(freq, 2)[None, :]
    return jnp.asarray(np.cos(angles)), jnp.asarray(np.sin(angles))


def retain(query, key, value, outgate, decay_rate, ret_gain):
    heads = decay_rate.shape[0]
    width = query.shape[1] // heads
    cosines, sines = tables(LEN, width)
    block = pl.BlockSpec((LEN, width), lambda h, s: (s, h))
    whole = pl.BlockSpec((LEN, width), lambda h, s: (0, 0))
    return pl.pallas_call(
        retain_kernel,
        grid=(heads, query.shape[0] // LEN),
        out_shape=jax.ShapeDtypeStruct(query.shape, BF16),
        in_specs=[
            pl.BlockSpec(memory_space=pltpu.SMEM), block, block, block, block, whole, whole,
            pl.BlockSpec((1, width), lambda h, s: (0, h)),
        ],
        out_specs=block,
        cost_estimate=cost(10**10),
        name="retain",
    )(decay_rate[:, None], query, key, value, outgate, cosines, sines, ret_gain[None])


def normed(full, gain):
    widened = full.astype(F32)
    mean = jnp.mean(widened * widened, axis=1, keepdims=True)
    return (widened * lax.rsqrt(mean + EPS) * gain).astype(BF16)


def dot(left, right):
    return jnp.dot(left, right, preferred_element_type=F32)


def ffn_part(features, gate, up, down, scale_gate, scale_up):
    hidden = jax.nn.silu(dot(features, gate) * scale_gate) * (dot(features, up) * scale_up)
    return dot(hidden.astype(BF16), down).astype(BF16)


def per_device(
    nfs, ntp,
    tokens, gain_one, w_gate, w_up, w_down, scale_gate, scale_up, scale_down,
    gain_mix, w_query, w_key, w_value, w_outgate,
    scale_query, scale_key, scale_value, scale_outgate,
    ret_gain, decay_rate, w_mix, scale_mix, gain_two,
):
    shards = [w.astype(BF16) for w in (w_query, w_key, w_value, w_outgate, w_mix)]
    gains = jnp.pad(jnp.stack((gain_one, gain_mix, gain_two)), ((0, 5), (0, 0)))
    gate, up, down, full, gains = enter(
        nfs, ntp, w_gate.astype(BF16), w_up.astype(BF16), w_down.astype(BF16), tokens, gains
    )
    part = ffn_part(normed(full, gains[0]), gate, up, down, scale_gate, scale_up)
    first, full, *weights, mix = combine(
        nfs, ntp, 1, 0.5, True, part, tokens, scale_down[None], shards, (0, 0, 0, 0, 1)
    )
    features = normed(full, gains[1])
    scales = (scale_query, scale_key, scale_value, scale_outgate)
    rows = [(dot(features, w) * s).astype(BF16) for w, s in zip(weights, scales)]
    mixed = retain(*rows, decay_rate, ret_gain)
    part = dot(mixed, mix).astype(BF16)
    second, full = combine(nfs, ntp, 2, 1.0, True, part, first, scale_mix[None])
    part = ffn_part(normed(full, gains[2]), gate, up, down, scale_gate, scale_up)
    return combine(nfs, ntp, 3, 0.5, False, part, second, scale_down[None])[0]


def solution(mesh):
    return jax.shard_map(
        functools.partial(per_device, mesh.shape["fs"], mesh.shape["tp"]),
        mesh=mesh,
        in_specs=(
            P("fs", "tp"),
            P("tp"),
            P("fs", "tp"),
            P("fs", "tp"),
            P("tp", "fs"),
            P("tp"),
            P("tp"),
            P("tp"),
            P("tp"),
            P("fs", "tp"),
            P("fs", "tp"),
            P("fs", "tp"),
            P("fs", "tp"),
            P("tp"),
            P("tp"),
            P("tp"),
            P("tp"),
            P("tp"),
            P("tp"),
            P("tp", "fs"),
            P("tp"),
            P("tp"),
        ),
        out_specs=P("fs", "tp"),
        check_vma=False,
    )
```
